32 devices in a mesh: rep: 2 (over x), fs: 8 (over z, y), tp: 2 (over core).
Axes of the slice: x: 2, y: 2, z: 4, core: 2. Of those that a mesh axis runs over, the one named last changes fastest.
Arguments:
- tokens: bfloat16 [16, 64, 2048], P(('rep', 'fs'), None, 'tp'), may hold values from -6 to 6
- lin_weight: bfloat16 [2048, 1024], P('fs', 'tp'), may hold values from -0.125 to 0.125
- glu_weight: bfloat16 [2048, 1024], P('fs', 'tp'), may hold values from -0.125 to 0.125
- conv_taps: float32 [31, 1024], P(None, 'tp'), may hold values from -4 to 4
- conv_gain: float32 [1024], P('tp'), may hold values from 0.1 to 1.9
- conv_out_weight: bfloat16 [1024, 2048], P('tp', 'fs'), may hold values from -0.1875 to 0.1875
- mix_gain: float32 [2048], replicated, may hold values from 0.1 to 1.9
- ff_gate: bfloat16 [2048, 5632], P('fs', 'tp'), may hold values from -0.125 to 0.125
- ff_up: bfloat16 [2048, 5632], P('fs', 'tp'), may hold values from -0.125 to 0.125
- ff_down: bfloat16 [5632, 2048], P('tp', 'fs'), may hold values from -0.078125 to 0.078125
- out_gain: float32 [2048], replicated, may hold values from 0.1 to 1.9
Outputs:
- encoded: bfloat16 [16, 64, 2048], P(('rep', 'fs'), None, 'tp')
The draws below stay inside these ranges and needn't reach their ends.
All inputs are finite; a program needn't handle non-finite values.
Results may differ from the reference program's by a relative error of at most 0.014.
Values may be sent and summed in bfloat16 or wider, within the bound.
No kernel may reach another device: no remote copies, remote signals or barrier semaphores. Data moves between devices by JAX's collectives and lax.ppermute only.
A program may use at most 128 MiB of HBM per device.

```python
import jax
import jax.numpy as jnp
from jax import lax

D = 2048
CONV = 1024
FF = 5632
TAPS = 31
TOK_DEV = 64
SEQUENCES = 16
N_TP = 2


def draw_conv_taps(key, part):
    first, second = jax.random.split(jax.random.fold_in(key, 17))
    channel = jnp.arange(CONV, dtype=jnp.float32)
    ramp = 3.0 ** (2.0 * channel / CONV - 1.0)
    spread = jnp.exp(jax.random.uniform(second, (CONV,), jnp.float32, -0.5, 0.5))
    base = jnp.clip(jax.random.normal(first, (TAPS, CONV), jnp.float32), -4.0, 4.0)
    return (base * TAPS ** (-0.5) * ramp * spread).astype(jnp.float32)


def shard_levels(key, shape, cuts, smallest, largest):
    def one(dim, parts):
        steps = jax.random.uniform(jax.random.fold_in(jax.random.fold_in(key, 6), dim), (parts,), jnp.float32, smallest / len(cuts), largest / len(cuts))
        return jnp.repeat(jnp.exp(steps), shape[dim] // parts).reshape((-1,) + (1,) * (len(shape) - dim - 1))

    factor_of = one(*cuts[0])
    for cut in cuts[1:]:
        factor_of = factor_of * one(*cut)
    return factor_of


def bell_draw(own_key, dims, deviation, bound, pieces=(), kind=jnp.bfloat16):
    values = deviation * jax.random.normal(own_key, dims, jnp.float32)
    if pieces:
        values = values * shard_levels(own_key, dims, pieces, -0.22, 0.18)
    return jnp.clip(values, -bound, bound).astype(kind)


def setup_inputs(seed: int = 0) -> dict:
    keys = jax.random.split(jax.random.key(seed), 12)
    return {
        "tokens": bell_draw(keys[0], (SEQUENCES, TOK_DEV, D), 1.0, 6.0, ((0, 16), (2, 2))),
        "lin_weight": bell_draw(keys[1], (D, CONV), D ** -0.5, 0.125, ((0, 8), (1, 2))),
        "glu_weight": bell_draw(keys[2], (D, CONV), D ** -0.5, 0.125, ((0, 8), (1, 2))),
        "conv_taps": draw_conv_taps(jax.random.fold_in(keys[11], 71), 0),
        "conv_gain": jnp.clip(1.0 + 0.18 * jax.random.normal(keys[4], (CONV,), jnp.float32), 0.1, 1.9),
        "conv_out_weight": bell_draw(keys[5], (CONV, D), CONV ** -0.5, 0.1875, ((0, 2), (1, 8))),
        "mix_gain": jnp.clip(1.0 + 0.18 * jax.random.normal(keys[6], (D,), jnp.float32), 0.1, 1.9),
        "ff_gate": bell_draw(keys[7], (D, FF), D ** -0.5, 0.125, ((0, 8), (1, 2))),
        "ff_up": bell_draw(keys[8], (D, FF), D ** -0.5, 0.125, ((0, 8), (1, 2))),
        "ff_down": bell_draw(keys[9], (FF, D), FF ** -0.5, 0.078125, ((0, 2), (1, 8))),
        "out_gain": jnp.clip(1.0 + 0.18 * jax.random.normal(keys[10], (D,), jnp.float32), 0.1, 1.9),
    }


residual_scale = 2.0 ** 0.25
epsilon = 1e-05

def rounded(value):
    return lax.optimization_barrier(value.astype(jnp.bfloat16)).astype(jnp.float32)

def normalize(values):
    average = lax.optimization_barrier(jnp.mean(values, axis=-1, keepdims=True))
    squares = lax.optimization_barrier(jnp.mean(values * values, axis=-1, keepdims=True))
    return (values - average) * lax.rsqrt(squares - average * average + epsilon)

def block_sum(left, right):
    rows, inner = left.shape
    width = inner // N_TP
    left_blocks = left.astype(jnp.float32).reshape(rows, N_TP, width)
    right_blocks = right.astype(jnp.float32).reshape(N_TP, width, right.shape[1])
    partial_value = jnp.einsum('tjc,jcd->jtd', left_blocks, right_blocks)
    return lax.optimization_barrier(jnp.sum(rounded(partial_value), axis=0))

def depthwise(values, conv_taps):
    margin = (TAPS - 1) // 2
    return lax.conv_general_dilated(values[None], conv_taps[:, None, :], (1,), [(margin, margin)], dimension_numbers=('NWC', 'WIO', 'NWC'), feature_group_count=values.shape[1], precision=lax.Precision.HIGHEST)[0]

def reference(tokens, lin_weight, glu_weight, conv_taps, conv_gain, conv_out_weight, mix_gain, ff_gate, ff_up, ff_down, out_gain):

    def one_sequence(inputs):
        linear = jnp.dot(inputs, lin_weight, preferred_element_type=jnp.float32)
        gating = jnp.dot(inputs, glu_weight, preferred_element_type=jnp.float32)
        glu = (linear * jax.nn.sigmoid(gating)).astype(jnp.bfloat16)
        conv = depthwise(glu.astype(jnp.float32), conv_taps)
        activated = jax.nn.silu(normalize(conv) * conv_gain).astype(jnp.bfloat16)
        mixed = rounded(block_sum(activated, conv_out_weight))
        middle = (normalize(residual_scale * inputs.astype(jnp.float32) + mixed) * mix_gain).astype(jnp.bfloat16)
        gate = jnp.dot(middle, ff_gate, preferred_element_type=jnp.float32)
        upward = jnp.dot(middle, ff_up, preferred_element_type=jnp.float32)
        hidden = (jax.nn.silu(gate) * upward).astype(jnp.bfloat16)
        forward = rounded(block_sum(hidden, ff_down))
        total = residual_scale * middle.astype(jnp.float32) + forward
        return (normalize(total) * out_gain).astype(jnp.bfloat16)
    return lax.map(one_sequence, tokens)
```

```python
import jax
import jax.numpy as jnp
from jax import lax
from jax.sharding import PartitionSpec as P

D = 2048
CONV = 1024
TAPS = 31


residual_scale = 2.0**0.25
epsilon = 1e-05


def rounded(value):
    return lax.optimization_barrier(value.astype(jnp.bfloat16)).astype(jnp.float32)


def scaled(values, totals, squares, count):
    average = totals[:, None] / count
    second = squares[:, None] / count
    return (values - average) * lax.rsqrt(second - average * average + epsilon)


def exchange(blocks, axis):
    return lax.all_to_all(blocks, axis, 0, 0)


def after(value, *earlier):
    return lax.optimization_barrier((value, *earlier))[0]


def sum_blocks(blocks):
    return jnp.sum(blocks.astype(jnp.float32), axis=0)


def on_device(
    tokens,
    lin_weight,
    glu_weight,
    conv_taps,
    conv_gain,
    conv_out_weight,
    mix_gain,
    ff_gate,
    ff_up,
    ff_down,
    out_gain,
):
    n_fs = lax.axis_size("fs")
    n_tp = lax.axis_size("tp")
    own_tokens = tokens[0]
    seq, feat_width = own_tokens.shape
    offset = lax.axis_index("tp") * feat_width
    width = feat_width * n_tp
    rows = lin_weight.shape[0]
    chans = lin_weight.shape[1]
    units = ff_gate.shape[1] // n_fs

    all_tokens = lax.all_gather(own_tokens, "tp", axis=1, tiled=True)
    row_tokens = exchange(all_tokens.reshape(seq, n_fs, rows).transpose(1, 0, 2), "fs")
    row_tokens = row_tokens.reshape(n_fs * seq, rows)

    def dealt_columns(weight):
        blocks = weight.reshape(rows, n_fs, units).transpose(1, 0, 2)
        return exchange(blocks, "fs").reshape(n_fs * rows, units)

    gate_own = dealt_columns(after(ff_gate, row_tokens))
    up_own = dealt_columns(after(ff_up, row_tokens))

    terms = jnp.concatenate(
        [
            jnp.dot(row_tokens, lin_weight, preferred_element_type=jnp.float32),
            jnp.dot(row_tokens, glu_weight, preferred_element_type=jnp.float32),
        ],
        axis=1,
    ).astype(jnp.bfloat16)
    both = sum_blocks(exchange(terms.reshape(n_fs, seq, 2 * chans), "fs"))
    down_blocks = after(ff_down, both).reshape(n_fs, units, ff_down.shape[1])
    down_own = exchange(down_blocks, "fs").transpose(1, 0, 2).reshape(units, width)

    glu = (both[:, :chans] * jax.nn.sigmoid(both[:, chans:])).astype(jnp.bfloat16)
    margin = (TAPS - 1) // 2
    conv = lax.conv_general_dilated(
        glu.astype(jnp.float32)[None],
        conv_taps[:, None, :],
        (1,),
        [(margin, margin)],
        dimension_numbers=("NWC", "WIO", "NWC"),
        feature_group_count=glu.shape[1],
        precision=lax.Precision.HIGHEST,
    )[0]
    conv_sums, conv_squares = lax.psum((jnp.sum(conv, axis=1), jnp.sum(conv * conv, axis=1)), "tp")
    activated = jax.nn.silu(scaled(conv, conv_sums, conv_squares, CONV) * conv_gain).astype(
        jnp.bfloat16
    )
    conv_terms = jnp.dot(
        activated,
        lax.all_gather(conv_out_weight, "fs", axis=1, tiled=True),
        preferred_element_type=jnp.float32,
    )
    mixed = rounded(
        lax.psum_scatter(
            conv_terms.astype(jnp.bfloat16), "tp", scatter_dimension=1, tiled=True
        ).astype(jnp.float32)
    )
    before = residual_scale * own_tokens.astype(jnp.float32) + mixed
    mix_sums, mix_squares = lax.psum(
        (jnp.sum(before, axis=1), jnp.sum(before * before, axis=1)), "tp"
    )
    gain_own = lax.dynamic_slice_in_dim(mix_gain, offset, feat_width, 0)
    middle_own = (scaled(before, mix_sums, mix_squares, D) * gain_own).astype(jnp.bfloat16)

    middle_half = lax.all_gather(middle_own, "fs", axis=0, tiled=True)
    middle_all = lax.all_gather(middle_half, "tp", axis=1, tiled=True)
    gate = jnp.dot(middle_all, gate_own, preferred_element_type=jnp.float32)
    upward = jnp.dot(middle_all, up_own, preferred_element_type=jnp.float32)
    hidden = (jax.nn.silu(gate) * upward).astype(jnp.bfloat16)
    down_terms = jnp.dot(hidden, down_own, preferred_element_type=jnp.float32)
    halves = down_terms.astype(jnp.bfloat16).reshape(n_fs * seq, n_tp, feat_width)
    over_tp = sum_blocks(exchange(halves.transpose(1, 0, 2), "tp")).astype(jnp.bfloat16)
    over_fs = sum_blocks(exchange(over_tp.reshape(n_fs, seq, feat_width), "fs"))
    forward = rounded(over_fs)
    final = residual_scale * middle_own.astype(jnp.float32) + forward
    out_sums, out_squares = lax.psum((jnp.sum(final, axis=1), jnp.sum(final * final, axis=1)), "tp")
    gain_slice = lax.dynamic_slice_in_dim(out_gain, offset, feat_width, 0)
    encoded = (scaled(final, out_sums, out_squares, D) * gain_slice).astype(jnp.bfloat16)
    return encoded[None]


def solution(mesh):
    return jax.shard_map(
        on_device,
        mesh=mesh,
        in_specs=(
            P(("rep", "fs"), None, "tp"),
            P("fs", "tp"),
            P("fs", "tp"),
            P(None, "tp"),
            P("tp"),
            P("tp", "fs"),
            P(),
            P("fs", "tp"),
            P("fs", "tp"),
            P("tp", "fs"),
            P(),
        ),
        out_specs=P(("rep", "fs"), None, "tp"),
        check_vma=False,
    )
```

```python
import jax
import jax.numpy as jnp
from jax import lax
from jax.sharding import PartitionSpec as P

D = 2048
CONV = 1024
TAPS = 31


residual_scale = 2.0**0.25
epsilon = 1e-05


def rounded(value):
    return lax.optimization_barrier(value.astype(jnp.bfloat16)).astype(jnp.float32)


def scaled(values, totals, squares, count):
    average = totals[:, None] / count
    second = squares[:, None] / count
    return (values - average) * lax.rsqrt(second - average * average + epsilon)


def exchange(blocks, axis):
    return lax.all_to_all(blocks, axis, 0, 0)


def after(value, *earlier):
    return lax.optimization_barrier((value, *earlier))[0]


def sum_blocks(blocks):
    return jnp.sum(blocks.astype(jnp.float32), axis=0)


def sent(value, axis, step):
    size = lax.axis_size(axis)
    return lax.ppermute(value, axis, [(i, (i + step) % size) for i in range(size)])


def tp_sum(terms):
    size = lax.axis_size("tp")
    own = lax.axis_index("tp")
    width = terms.shape[1] // size

    def part(step):
        return lax.dynamic_slice_in_dim(terms, (own + step) % size * width, width, 1)

    total = part(0).astype(jnp.float32)
    for step in range(1, size):
        total = total + sent(part(step), "tp", step).astype(jnp.float32)
    return total


def fs_grid():
    size = lax.axis_size("fs")
    outer = 2 ** (size.bit_length() // 2)
    if size % outer:
        outer = 1
    return outer, size // outer


def grid_sent(value, d_out, d_in):
    outer, inner = fs_grid()
    pairs = [
        (o * inner + i, (o + d_out) % outer * inner + (i + d_in) % inner)
        for o in range(outer)
        for i in range(inner)
    ]
    return lax.ppermute(value, "fs", pairs)


def fs_gather(block):
    outer, inner = fs_grid()
    near = [grid_sent(block, 0, i) for i in range(1, inner)]
    far = [block] + [grid_sent(block, o, 0) for o in range(1, outer)]
    rest = jnp.concatenate(far[1:]) if outer > 1 else None
    parts = list(far)
    for i in range(1, inner):
        parts.append(near[i - 1])
        if rest is not None:
            parts.append(grid_sent(rest, 0, i))
    return jnp.concatenate(parts)


def fs_scatter_sum(blocks):
    outer, inner = fs_grid()
    rows = blocks.shape[0] // (outer * inner)
    parts = blocks.reshape(inner, outer * rows, blocks.shape[1])
    if outer > 1:
        far = parts[0, rows:].astype(jnp.float32)
        for i in range(1, inner):
            far = far + grid_sent(parts[i, rows:], 0, -i).astype(jnp.float32)
        far = far.astype(jnp.bfloat16)
    total = parts[0, :rows].astype(jnp.float32)
    for i in range(1, inner):
        total = total + grid_sent(parts[i, :rows], 0, -i).astype(jnp.float32)
    for o in range(1, outer):
        total = total + grid_sent(far[(o - 1) * rows : o * rows], -o, 0).astype(jnp.float32)
    return total


def on_device(
    tokens,
    lin_weight,
    glu_weight,
    conv_taps,
    conv_gain,
    conv_out_weight,
    mix_gain,
    ff_gate,
    ff_up,
    ff_down,
    out_gain,
):
    n_fs = lax.axis_size("fs")
    n_tp = lax.axis_size("tp")
    own_tokens = tokens[0]
    seq, feat_width = own_tokens.shape
    offset = lax.axis_index("tp") * feat_width
    width = feat_width * n_tp
    rows = lin_weight.shape[0]
    chans = lin_weight.shape[1]
    units = ff_gate.shape[1] // n_fs

    all_tokens = lax.all_gather(own_tokens, "tp", axis=1, tiled=True)
    row_tokens = exchange(all_tokens.reshape(seq, n_fs, rows).transpose(1, 0, 2), "fs")
    row_tokens = row_tokens.reshape(n_fs * seq, rows)

    terms = jnp.concatenate(
        [
            jnp.dot(row_tokens, lin_weight, preferred_element_type=jnp.float32),
            jnp.dot(row_tokens, glu_weight, preferred_element_type=jnp.float32),
        ],
        axis=1,
    ).astype(jnp.bfloat16)
    both = sum_blocks(exchange(terms.reshape(n_fs, seq, 2 * chans), "fs"))

    n_rep = lax.axis_size("rep")
    share = units // n_rep
    rep = lax.axis_index("rep")

    def passed_on(received):
        return [received] + [sent(received, "rep", step) for step in range(1, n_rep)]

    def own_share(weight):
        split = weight.reshape(rows, n_fs, n_rep, share)
        return lax.dynamic_index_in_dim(split, rep, 2, keepdims=False)

    pair = jnp.concatenate([own_share(ff_gate), own_share(ff_up)], axis=2).transpose(1, 0, 2)
    first_blocks, second_blocks = pair[:, : rows // 2], pair[:, rows // 2 :]
    first = exchange(after(first_blocks, both), "fs")
    second = exchange(after(second_blocks, first), "fs")
    down_share = lax.dynamic_index_in_dim(
        ff_down.reshape(n_fs, n_rep, share, rows), rep, 1, keepdims=False
    )
    down_first = exchange(after(down_share, second), "fs")
    down_parts = passed_on(down_first.transpose(1, 0, 2).reshape(share, width))
    pair_parts = [
        jnp.concatenate(halves, axis=1) for halves in zip(passed_on(first), passed_on(second))
    ]

    glu = (both[:, :chans] * jax.nn.sigmoid(both[:, chans:])).astype(jnp.bfloat16)
    margin = (TAPS - 1) // 2
    conv = lax.conv_general_dilated(
        glu.astype(jnp.float32)[None],
        conv_taps[:, None, :],
        (1,),
        [(margin, margin)],
        dimension_numbers=("NWC", "WIO", "NWC"),
        feature_group_count=glu.shape[1],
        precision=lax.Precision.HIGHEST,
    )[0]
    conv_sums, conv_squares = lax.psum((jnp.sum(conv, axis=1), jnp.sum(conv * conv, axis=1)), "tp")
    activated = jax.nn.silu(scaled(conv, conv_sums, conv_squares, CONV) * conv_gain).astype(
        jnp.bfloat16
    )
    strip = chans // n_rep
    own_strip = lax.dynamic_slice_in_dim(conv_out_weight, rep * strip, strip, 0)
    conv_terms = 0.0
    for step, strip_weight in enumerate(
        passed_on(lax.all_gather(own_strip, "fs", axis=1, tiled=True))
    ):
        conv_terms = conv_terms + jnp.dot(
            lax.dynamic_slice_in_dim(activated, (rep - step) % n_rep * strip, strip, 1),
            strip_weight,
            preferred_element_type=jnp.float32,
        )
    mixed = rounded(tp_sum(conv_terms.astype(jnp.bfloat16)))
    before = residual_scale * own_tokens.astype(jnp.float32) + mixed
    mix_sums, mix_squares = lax.psum(
        (jnp.sum(before, axis=1), jnp.sum(before * before, axis=1)), "tp"
    )
    gain_own = lax.dynamic_slice_in_dim(mix_gain, offset, feat_width, 0)
    middle_own = (scaled(before, mix_sums, mix_squares, D) * gain_own).astype(jnp.bfloat16)

    middle_half = fs_gather(middle_own)
    tp = lax.axis_index("tp")
    columns = [(middle_half, tp)] + [
        (sent(middle_half, "tp", step), (tp - step) % n_tp) for step in range(1, n_tp)
    ]
    down_terms = 0.0
    per_tp = n_fs // n_tp
    for pair_weight, down_weight in zip(pair_parts, down_parts):
        lifted = 0.0
        for half, index in columns:
            weight = lax.dynamic_slice_in_dim(pair_weight, index * per_tp, per_tp, 0)
            lifted = lifted + jnp.dot(
                half, weight.reshape(feat_width, 2 * share), preferred_element_type=jnp.float32
            )
        hidden = (jax.nn.silu(lifted[:, :share]) * lifted[:, share:]).astype(jnp.bfloat16)
        down_terms = down_terms + jnp.dot(
            hidden, down_weight, preferred_element_type=jnp.float32
        )
    over_tp = tp_sum(down_terms.astype(jnp.bfloat16)).astype(jnp.bfloat16)
    forward = rounded(fs_scatter_sum(over_tp))
    final = residual_scale * middle_own.astype(jnp.float32) + forward
    out_sums, out_squares = lax.psum((jnp.sum(final, axis=1), jnp.sum(final * final, axis=1)), "tp")
    gain_slice = lax.dynamic_slice_in_dim(out_gain, offset, feat_width, 0)
    encoded = (scaled(final, out_sums, out_squares, D) * gain_slice).astype(jnp.bfloat16)
    return encoded[None]


def solution(mesh):
    return jax.shard_map(
        on_device,
        mesh=mesh,
        in_specs=(
            P(("rep", "fs"), None, "tp"),
            P("fs", "tp"),
            P("fs", "tp"),
            P(None, "tp"),
            P("tp"),
            P("tp", "fs"),
            P(),
            P("fs", "tp"),
            P("fs", "tp"),
            P("tp", "fs"),
            P(),
        ),
        out_specs=P(("rep", "fs"), None, "tp"),
        check_vma=False,
    )
```

```python
import jax
import jax.numpy as jnp
from jax import lax
from jax.sharding import PartitionSpec as P


D = 2048
CONV = 1024
TAPS = 31


residual_scale = 2.0**0.25
epsilon = 1e-05


def rounded(value):
    return lax.optimization_barrier(value.astype(jnp.bfloat16)).astype(jnp.float32)


def scaled(values, totals, squares, count):
    average = totals[:, None] / count
    second = squares[:, None] / count
    return (values - average) * lax.rsqrt(second - average * average + epsilon)


def exchange(blocks, axis):
    return lax.all_to_all(blocks, axis, 0, 0)


def after(value, *earlier):
    return lax.optimization_barrier((value, *earlier))[0]


def sum_blocks(blocks):
    return jnp.sum(blocks.astype(jnp.float32), axis=0)


def sent(value, axis, step):
    size = lax.axis_size(axis)
    return lax.ppermute(value, axis, [(i, (i + step) % size) for i in range(size)])


def tp_sum(terms):
    size = lax.axis_size("tp")
    own = lax.axis_index("tp")
    width = terms.shape[1] // size

    def part(step):
        return lax.dynamic_slice_in_dim(terms, (own + step) % size * width, width, 1)

    total = part(0).astype(jnp.float32)
    for step in range(1, size):
        total = total + sent(part(step), "tp", step).astype(jnp.float32)
    return total


def exchange_by_permutes(blocks, axis):
    size = lax.axis_size(axis)
    own = lax.axis_index(axis)
    received = blocks
    for step in range(1, size):
        block = lax.dynamic_index_in_dim(blocks, (own + step) % size, 0, keepdims=False)
        received = lax.dynamic_update_index_in_dim(
            received, sent(block, axis, step), (own - step) % size, 0
        )
    return received


def fs_grid():
    size = lax.axis_size("fs")
    outer = 2 ** (size.bit_length() // 2)
    if size % outer:
        outer = 1
    return outer, size // outer


def grid_sent(value, d_out, d_in):
    outer, inner = fs_grid()
    pairs = [
        (o * inner + i, (o + d_out) % outer * inner + (i + d_in) % inner)
        for o in range(outer)
        for i in range(inner)
    ]
    return lax.ppermute(value, "fs", pairs)


def fs_gather(block):
    outer, inner = fs_grid()
    near = [grid_sent(block, 0, i) for i in range(1, inner)]
    far = [block] + [grid_sent(block, o, 0) for o in range(1, outer)]
    rest = jnp.concatenate(far[1:]) if outer > 1 else None
    parts = list(far)
    for i in range(1, inner):
        parts.append(near[i - 1])
        if rest is not None:
            parts.append(grid_sent(rest, 0, i))
    return jnp.concatenate(parts)


def fs_scatter_sum(blocks):
    outer, inner = fs_grid()
    rows = blocks.shape[0] // (outer * inner)
    parts = blocks.reshape(inner, outer * rows, blocks.shape[1])
    if outer > 1:
        far = parts[0, rows:].astype(jnp.float32)
        for i in range(1, inner):
            far = far + grid_sent(parts[i, rows:], 0, -i).astype(jnp.float32)
        far = far.astype(jnp.bfloat16)
    total = parts[0, :rows].astype(jnp.float32)
    for i in range(1, inner):
        total = total + grid_sent(parts[i, :rows], 0, -i).astype(jnp.float32)
    for o in range(1, outer):
        total = total + grid_sent(far[(o - 1) * rows : o * rows], -o, 0).astype(jnp.float32)
    return total


def on_device(
    tokens,
    lin_weight,
    glu_weight,
    conv_taps,
    conv_gain,
    conv_out_weight,
    mix_gain,
    ff_gate,
    ff_up,
    ff_down,
    out_gain,
):
    n_fs = lax.axis_size("fs")
    n_tp = lax.axis_size("tp")
    own_tokens = tokens[0]
    seq, feat_width = own_tokens.shape
    offset = lax.axis_index("tp") * feat_width
    width = feat_width * n_tp
    rows = lin_weight.shape[0]
    chans = lin_weight.shape[1]
    units = ff_gate.shape[1] // n_fs

    all_tokens = lax.all_gather(own_tokens, "tp", axis=1, tiled=True)
    row_tokens = exchange(all_tokens.reshape(seq, n_fs, rows).transpose(1, 0, 2), "fs")
    row_tokens = row_tokens.reshape(n_fs * seq, rows)

    terms = jnp.concatenate(
        [
            jnp.dot(row_tokens, lin_weight, preferred_element_type=jnp.float32),
            jnp.dot(row_tokens, glu_weight, preferred_element_type=jnp.float32),
        ],
        axis=1,
    ).astype(jnp.bfloat16)
    both = sum_blocks(exchange(terms.reshape(n_fs, seq, 2 * chans), "fs"))

    n_rep = lax.axis_size("rep")
    share = units // n_rep
    rep = lax.axis_index("rep")

    def passed_on(received):
        return [received] + [sent(received, "rep", step) for step in range(1, n_rep)]

    def own_share(weight):
        split = weight.reshape(rows, n_fs, n_rep, share)
        return lax.dynamic_index_in_dim(split, rep, 2, keepdims=False)

    pair = jnp.concatenate([own_share(ff_gate), own_share(ff_up)], axis=2).transpose(1, 0, 2)
    first_blocks, second_blocks = pair[:, : rows // 2], pair[:, rows // 2 :]
    first = exchange_by_permutes(after(first_blocks, all_tokens), "fs")
    second = exchange(after(second_blocks, both), "fs")
    down_share = lax.dynamic_index_in_dim(
        ff_down.reshape(n_fs, n_rep, share, rows), rep, 1, keepdims=False
    )
    down_first = exchange(after(down_share, second), "fs")
    down_parts = passed_on(down_first.transpose(1, 0, 2).reshape(share, width))
    pair_parts = [
        jnp.concatenate(halves, axis=1) for halves in zip(passed_on(first), passed_on(second))
    ]

    glu = (both[:, :chans] * jax.nn.sigmoid(both[:, chans:])).astype(jnp.bfloat16)
    margin = (TAPS - 1) // 2
    conv = lax.conv_general_dilated(
        glu.astype(jnp.float32)[None],
        conv_taps[:, None, :],
        (1,),
        [(margin, margin)],
        dimension_numbers=("NWC", "WIO", "NWC"),
        feature_group_count=glu.shape[1],
        precision=lax.Precision.HIGHEST,
    )[0]
    conv_sums, conv_squares = lax.psum((jnp.sum(conv, axis=1), jnp.sum(conv * conv, axis=1)), "tp")
    activated = jax.nn.silu(scaled(conv, conv_sums, conv_squares, CONV) * conv_gain).astype(
        jnp.bfloat16
    )
    conv_terms = jnp.dot(
        activated,
        lax.all_gather(conv_out_weight, "fs", axis=1, tiled=True),
        preferred_element_type=jnp.float32,
    )
    mixed = rounded(tp_sum(conv_terms.astype(jnp.bfloat16)))
    before = residual_scale * own_tokens.astype(jnp.float32) + mixed
    mix_sums, mix_squares = lax.psum(
        (jnp.sum(before, axis=1), jnp.sum(before * before, axis=1)), "tp"
    )
    gain_own = lax.dynamic_slice_in_dim(mix_gain, offset, feat_width, 0)
    middle_own = (scaled(before, mix_sums, mix_squares, D) * gain_own).astype(jnp.bfloat16)

    middle_half = fs_gather(middle_own)
    tp = lax.axis_index("tp")
    columns = [(middle_half, tp)] + [
        (sent(middle_half, "tp", step), (tp - step) % n_tp) for step in range(1, n_tp)
    ]
    down_terms = 0.0
    per_tp = n_fs // n_tp
    for pair_weight, down_weight in zip(pair_parts, down_parts):
        lifted = 0.0
        for half, index in columns:
            weight = lax.dynamic_slice_in_dim(pair_weight, index * per_tp, per_tp, 0)
            lifted = lifted + jnp.dot(
                half, weight.reshape(feat_width, 2 * share), preferred_element_type=jnp.float32
            )
        hidden = (jax.nn.silu(lifted[:, :share]) * lifted[:, share:]).astype(jnp.bfloat16)
        down_terms = down_terms + jnp.dot(
            hidden, down_weight, preferred_element_type=jnp.float32
        )
    over_tp = tp_sum(down_terms.astype(jnp.bfloat16)).astype(jnp.bfloat16)
    forward = rounded(fs_scatter_sum(over_tp))
    final = residual_scale * middle_own.astype(jnp.float32) + forward
    out_sums, out_squares = lax.psum((jnp.sum(final, axis=1), jnp.sum(final * final, axis=1)), "tp")
    gain_slice = lax.dynamic_slice_in_dim(out_gain, offset, feat_width, 0)
    encoded = (scaled(final, out_sums, out_squares, D) * gain_slice).astype(jnp.bfloat16)
    return encoded[None]


def solution(mesh):
    return jax.shard_map(
        on_device,
        mesh=mesh,
        in_specs=(
            P(("rep", "fs"), None, "tp"),
            P("fs", "tp"),
            P("fs", "tp"),
            P(None, "tp"),
            P("tp"),
            P("tp", "fs"),
            P(),
            P("fs", "tp"),
            P("fs", "tp"),
            P("tp", "fs"),
            P(),
        ),
        out_specs=P(("rep", "fs"), None, "tp"),
        check_vma=False,
    )
```
